32 devices in a mesh: tp: 32 (over z, y, x, core).
Axes of the slice: x: 2, y: 2, z: 4, core: 2. Of those that a mesh axis runs over, the one named last changes fastest.
Arguments:
- tokens: bfloat16 [128, 4096], P(None, 'tp'), may hold values from -6 to 6
- norm_gain: float32 [2, 4096], replicated, may hold values from 0.5 to 1.5
- norm_bias: float32 [2, 4096], replicated, may hold values from -0.4 to 0.4
- input_weight: bfloat16 [2, 4096, 2048], P(None, None, 'tp'), may hold values from -0.1875 to 0.1875
- gate_weight: bfloat16 [2, 4096, 4096], P(None, None, 'tp'), may hold values from -0.1875 to 0.1875
- decay_real: float32 [2, 8192], P(None, 'tp'), may hold values from -1 to -0.2
- decay_imag: float32 [2, 8192], P(None, 'tp'), may hold values from -0.5 to 198.5, as said below
- log_step: float32 [2, 128], P(None, 'tp'), may hold values from -1.6 to 0
- input_coef_real: float32 [2, 8192, 16], P(None, 'tp'), may hold values from -3 to 3
- input_coef_imag: float32 [2, 8192, 16], P(None, 'tp'), may hold values from -3 to 3
- output_coef_real: float32 [2, 8192, 16], P(None, 'tp'), may hold values from -0.5 to 0.5
- output_coef_imag: float32 [2, 8192, 16], P(None, 'tp'), may hold values from -0.5 to 0.5
- skip_coef: float32 [2, 2048], P(None, 'tp'), may hold values from -4 to 4
- value_weight: bfloat16 [2, 2048, 4096], P(None, None, 'tp'), may hold values from -0.25 to 0.25
- gating_weight: bfloat16 [2, 2048, 4096], P(None, None, 'tp'), may hold values from -0.25 to 0.25
- output_weight: bfloat16 [2, 4096, 4096], P(None, 'tp'), may hold values from -0.5 to 0.5
- state_real: float32 [2, 128, 8192], P(None, None, 'tp'), may hold values from -3 to 3
- state_imag: float32 [2, 128, 8192], P(None, None, 'tp'), may hold values from -3 to 3
Outputs:
- block_output: bfloat16 [128, 4096], P(None, 'tp')
- new_state_real: float32 [2, 128, 8192], P(None, None, 'tp')
- new_state_imag: float32 [2, 128, 8192], P(None, None, 'tp')
The draws below stay inside these ranges and needn't reach their ends.
Inputs may be any that keep to these rules, and one draw needn't show every extreme that they name: `decay_imag`: entry j of every block lies within 0.5 of pi times (j mod 64).
All inputs are finite; a program needn't handle non-finite values.
Results may differ from the reference program's by a relative error of at most 0.025.
Values may be sent and summed in bfloat16 or wider, within the bound.
A program may use at most 64 MiB of HBM per device.

```python
import math
import jax
import jax.numpy as jnp
from jax import lax

MODEL_WIDTH = 4096
SSM_WIDTH = 2048
GROUP_WIDTH = 16
STATE_SIZE = 64
BLOCKS = 2
SEQUENCES = 128
GROUPS = 128


def draw_decay_imag(key, part):
    positions = jnp.arange(GROUPS * STATE_SIZE) % STATE_SIZE
    centers = math.pi * positions.astype(jnp.float32)
    jitter = 0.2 * jax.random.normal(key, (BLOCKS, GROUPS * STATE_SIZE), jnp.float32)
    jitter = jnp.clip(jitter, -0.5, 0.5)
    return centers[None, :] + jitter


def strengthened(values, rng, source, target, shards_of, factor):
    owner, partner = [(jnp.arange(values.shape[position]) // (values.shape[position] // shards_of)).reshape([-1 if axis == position else 1 for axis in range(values.ndim)]) for position in (source, target)]
    chosen = jax.random.permutation(rng, shards_of)[partner]
    strong = (owner == chosen) | (owner == (partner + shards_of // 2) % shards_of)
    return jnp.where(strong, factor * values, values)


def level_of(key, shape, shards, least, top_value):
    level, own = 1.0, jax.random.fold_in(key, 6)
    for dim, parts in shards:
        heights = jnp.exp(jax.random.uniform(jax.random.fold_in(own, dim), (parts,), jnp.float32, least / len(shards), top_value / len(shards)))
        level = level * jnp.repeat(heights, shape[dim] // parts).reshape([-1 if axis == dim else 1 for axis in range(len(shape))])
    return level


def centred(rng, dims, scale, limit, pieces=(), kind=jnp.bfloat16):
    drawn = scale * jax.random.normal(rng, dims, jnp.float32)
    if pieces:
        drawn = drawn * level_of(rng, dims, pieces, -0.22, 0.18)
    return jnp.clip(drawn, -limit, limit).astype(kind)


def heavy_noise(own_key, extent, scale, bound, cuts, heavy, dtype=jnp.bfloat16):
    array = scale * jax.random.normal(own_key, extent, jnp.float32)
    if cuts:
        array = array * level_of(own_key, extent, cuts, -0.22, 0.18)
    return jnp.clip(strengthened(array, jax.random.fold_in(own_key, 3), *heavy), -bound, bound).astype(dtype)


def setup_inputs(seed: int = 0) -> dict:
    keys = jax.random.split(jax.random.key(seed), 19)
    return {
        "tokens": centred(keys[0], (SEQUENCES, MODEL_WIDTH), 1.0, 6.0, ((1, 32),)),
        "norm_gain": jnp.clip(1.0 + 0.1 * jax.random.normal(keys[1], (BLOCKS, MODEL_WIDTH), jnp.float32), 0.5, 1.5),
        "norm_bias": centred(keys[2], (BLOCKS, MODEL_WIDTH), 0.1, 0.4, (), jnp.float32),
        "input_weight": heavy_noise(keys[3], (BLOCKS, MODEL_WIDTH, SSM_WIDTH), MODEL_WIDTH ** -0.5, 0.1875, ((2, 32),), (1, 2, 32, 2.75)),
        "gate_weight": heavy_noise(keys[4], (BLOCKS, MODEL_WIDTH, MODEL_WIDTH), MODEL_WIDTH ** -0.5, 0.1875, ((2, 32),), (1, 2, 32, 2.75)),
        "decay_real": jnp.clip(-1.0 + 0.8 * jax.random.uniform(keys[5], (BLOCKS, GROUPS * STATE_SIZE), jnp.float32) ** level_of(keys[5], (BLOCKS, GROUPS * STATE_SIZE), ((1, 32),), -0.2, 0.2), -1.0, -0.2),
        "decay_imag": draw_decay_imag(jax.random.fold_in(keys[18], 71), 0),
        "log_step": jnp.clip(-1.6 + 1.6 * jax.random.uniform(keys[7], (BLOCKS, GROUPS), jnp.float32) ** level_of(keys[7], (BLOCKS, GROUPS), ((1, 32),), -0.2, 0.2), -1.6, 0.0),
        "input_coef_real": centred(keys[8], (BLOCKS, GROUPS * STATE_SIZE, GROUP_WIDTH), (GROUP_WIDTH // 4) ** -0.5, 3.0, ((1, 32),), jnp.float32),
        "input_coef_imag": centred(keys[9], (BLOCKS, GROUPS * STATE_SIZE, GROUP_WIDTH), (GROUP_WIDTH // 4) ** -0.5, 3.0, ((1, 32),), jnp.float32),
        "output_coef_real": centred(keys[10], (BLOCKS, GROUPS * STATE_SIZE, GROUP_WIDTH), (2 * STATE_SIZE) ** -0.5, 0.5, ((1, 32),), jnp.float32),
        "output_coef_imag": centred(keys[11], (BLOCKS, GROUPS * STATE_SIZE, GROUP_WIDTH), (2 * STATE_SIZE) ** -0.5, 0.5, ((1, 32),), jnp.float32),
        "skip_coef": centred(keys[12], (BLOCKS, SSM_WIDTH), 1.0, 4.0, ((1, 32),), jnp.float32),
        "value_weight": heavy_noise(keys[13], (BLOCKS, SSM_WIDTH, MODEL_WIDTH), SSM_WIDTH ** -0.5, 0.25, ((2, 32),), (1, 2, 32, 2.75)),
        "gating_weight": heavy_noise(keys[14], (BLOCKS, SSM_WIDTH, MODEL_WIDTH), SSM_WIDTH ** -0.5, 0.25, ((2, 32),), (1, 2, 32, 2.75)),
        "output_weight": heavy_noise(keys[15], (BLOCKS, MODEL_WIDTH, MODEL_WIDTH), (MODEL_WIDTH // 8) ** -0.5, 0.5, ((1, 32),), (1, 2, 32, 2.75)),
        "state_real": centred(keys[16], (BLOCKS, SEQUENCES, GROUPS * STATE_SIZE), 0.5, 3.0, ((2, 32),), jnp.float32),
        "state_imag": centred(keys[17], (BLOCKS, SEQUENCES, GROUPS * STATE_SIZE), 0.5, 3.0, ((2, 32),), jnp.float32),
    }


norm_eps = 1e-05
highest = lax.Precision.HIGHEST

def layer_norm(values, scales, offsets):
    widened = values.astype(jnp.float32)
    center = lax.optimization_barrier(jnp.mean(widened, axis=-1, keepdims=True))
    spread = lax.optimization_barrier(jnp.mean(jnp.square(widened - center), axis=-1, keepdims=True))
    normed = (widened - center) * lax.rsqrt(spread + norm_eps) * scales + offsets
    return normed.astype(jnp.bfloat16)

def discretize(decay_real, decay_imag, step_size, coef_real, coef_imag):
    growth = jnp.exp(decay_real * step_size)
    angles = decay_imag * step_size
    bar_real = growth * jnp.cos(angles)
    bar_imag = growth * jnp.sin(angles)
    modulus = decay_real * decay_real + decay_imag * decay_imag
    minus_real = bar_real - 1.0
    hold_real = (minus_real * decay_real + bar_imag * decay_imag) / modulus
    hold_imag = (bar_imag * decay_real - minus_real * decay_imag) / modulus
    coupling_real = hold_real[:, None] * coef_real - hold_imag[:, None] * coef_imag
    coupling_imag = hold_real[:, None] * coef_imag + hold_imag[:, None] * coef_real
    return (bar_real, bar_imag, coupling_real, coupling_imag)

def mixer_block(inputs, norm_gain, norm_bias, input_weight, gate_weight, decay_real, decay_imag, log_step, input_coef_real, input_coef_imag, output_coef_real, output_coef_imag, skip_coef, value_weight, gating_weight, output_weight, state_real, state_imag):
    batch_rows = inputs.shape[0]
    normed = layer_norm(inputs, norm_gain, norm_bias)
    drives = jnp.dot(normed, input_weight, preferred_element_type=jnp.float32).astype(jnp.bfloat16)
    gate_rows = jnp.dot(normed, gate_weight, preferred_element_type=jnp.float32).astype(jnp.bfloat16)
    step_size = jnp.repeat(jnp.exp(log_step), STATE_SIZE)
    bar_real, bar_imag, coupling_real, coupling_imag = discretize(decay_real, decay_imag, step_size, input_coef_real, input_coef_imag)
    grouped = drives.astype(jnp.float32).reshape(batch_rows, GROUPS, GROUP_WIDTH)
    push_real = jnp.einsum('bgc,gpc->bgp', grouped, coupling_real.reshape(GROUPS, STATE_SIZE, GROUP_WIDTH), precision=highest).reshape(batch_rows, GROUPS * STATE_SIZE)
    push_imag = jnp.einsum('bgc,gpc->bgp', grouped, coupling_imag.reshape(GROUPS, STATE_SIZE, GROUP_WIDTH), precision=highest).reshape(batch_rows, GROUPS * STATE_SIZE)
    fresh_real = bar_real * state_real - bar_imag * state_imag + push_real
    fresh_imag = bar_real * state_imag + bar_imag * state_real + push_imag
    readout = jnp.einsum('bgp,gpc->bgc', fresh_real.reshape(batch_rows, GROUPS, STATE_SIZE), output_coef_real.reshape(GROUPS, STATE_SIZE, GROUP_WIDTH), precision=highest)
    readout = readout - jnp.einsum('bgp,gpc->bgc', fresh_imag.reshape(batch_rows, GROUPS, STATE_SIZE), output_coef_imag.reshape(GROUPS, STATE_SIZE, GROUP_WIDTH), precision=highest)
    readout = readout.reshape(batch_rows, SSM_WIDTH) + skip_coef * drives.astype(jnp.float32)
    activated = jax.nn.gelu(readout).astype(jnp.bfloat16)
    values = jnp.dot(activated, value_weight, preferred_element_type=jnp.float32).astype(jnp.bfloat16)
    gating = jnp.dot(activated, gating_weight, preferred_element_type=jnp.float32).astype(jnp.bfloat16)
    mixture = (jax.nn.sigmoid(gate_rows.astype(jnp.float32)) * values.astype(jnp.float32) * jax.nn.sigmoid(gating.astype(jnp.float32))).astype(jnp.bfloat16)
    output = jnp.dot(mixture, output_weight, preferred_element_type=jnp.float32).astype(jnp.bfloat16)
    return (output, fresh_real, fresh_imag)

def reference(tokens, norm_gain, norm_bias, input_weight, gate_weight, decay_real, decay_imag, log_step, input_coef_real, input_coef_imag, output_coef_real, output_coef_imag, skip_coef, value_weight, gating_weight, output_weight, state_real, state_imag):
    current = tokens
    new_reals = []
    new_imags = []
    for block_index in range(BLOCKS):
        current, fresh_real, fresh_imag = mixer_block(current, norm_gain[block_index], norm_bias[block_index], input_weight[block_index], gate_weight[block_index], decay_real[block_index], decay_imag[block_index], log_step[block_index], input_coef_real[block_index], input_coef_imag[block_index], output_coef_real[block_index], output_coef_imag[block_index], skip_coef[block_index], value_weight[block_index], gating_weight[block_index], output_weight[block_index], state_real[block_index], state_imag[block_index])
        new_reals.append(fresh_real)
        new_imags.append(fresh_imag)
    return (current, jnp.stack(new_reals), jnp.stack(new_imags))
```

```python
from functools import partial

import jax
import jax.numpy as jnp
from jax import lax
from jax.experimental import pallas as pl
from jax.experimental.pallas import tpu as pltpu
from jax.sharding import PartitionSpec as P

GROUP_WIDTH = 16
STATE_SIZE = 64
BLOCKS = 2
PLANE = 4

norm_eps = 1e-05
highest = lax.Precision.HIGHEST
f32 = jnp.float32
bf16 = jnp.bfloat16


def kernel(
    depth,
    tokens,
    norm_gain,
    norm_bias,
    decay_real,
    decay_imag,
    log_step,
    in_real,
    in_imag,
    out_real,
    out_imag,
    skip_coef,
    input_hbm,
    gate_hbm,
    value_hbm,
    gating_hbm,
    output_hbm,
    state_real_hbm,
    state_imag_hbm,
    block_output,
    new_real_hbm,
    new_imag_hbm,
    input_w,
    gate_w,
    value_w,
    gating_w,
    output_w,
    held_real,
    held_imag,
    whole,
    normed,
    current,
    half,
    acts,
    push_w,
    read_w,
    partial_sums,
    from_core,
    merged,
    from_plane,
    upper,
    from_line,
    load_sem,
    store_sem,
    pair_send,
    pair_recv,
    ga_send,
    ga_recv,
    rs_send,
    rs_recv,
):
    rows, cols = tokens.shape
    channels = skip_coef.shape[1]
    states = decay_real.shape[1]
    groups = channels // GROUP_WIDTH
    span = 2 * channels
    upper_rows = rows // 2

    me = lax.axis_index("tp")
    core = lax.rem(me, 2)
    chip = me // 2
    spot = lax.rem(chip, PLANE)
    level = chip // PLANE
    partner = chip * 2 + (1 - core)

    def chip_at(lev, place):
        return lev * PLANE + place

    def shifted(step):
        return lax.rem(level + step, depth)

    def mirrored(code):
        if code == 0:
            return spot
        x, y = lax.rem(spot, 2), spot // 2
        if code & 1:
            x = 1 - x
        if code & 2:
            y = 1 - y
        return y * 2 + x

    line_peers = [chip_at(shifted(s), spot) * 2 + core for s in range(1, depth)]
    plane_peers = [chip_at(level, mirrored(c)) * 2 + core for c in range(1, PLANE)]

    loads = []
    weights = (
        (input_hbm, input_w),
        (gate_hbm, gate_w),
        (state_real_hbm, held_real),
        (state_imag_hbm, held_imag),
        (value_hbm, value_w),
        (gating_hbm, gating_w),
        (output_hbm, output_w),
    )
    for b in range(BLOCKS):
        block_loads = []
        for i, (src, dst) in enumerate(weights):
            copy = pltpu.make_async_copy(src.at[b], dst.at[b], load_sem.at[b, i])
            copy.start()
            block_loads.append(copy)
        loads.append(block_loads)

    barrier = pltpu.get_barrier_semaphore()
    everyone = line_peers + plane_peers + [partner]
    for peer in everyone:
        pl.semaphore_signal(
            barrier, inc=1, device_id=(peer,), device_id_type=pl.DeviceIdType.MESH
        )
    pl.semaphore_wait(barrier, len(everyone))

    def remote(src, dst, send, recv, peer):
        return pltpu.make_async_remote_copy(
            src_ref=src,
            dst_ref=dst,
            send_sem=send,
            recv_sem=recv,
            device_id=(peer,),
            device_id_type=pl.DeviceIdType.MESH,
        )

    order = sorted(range(depth), key=lambda s: min(s, depth - s))

    def gather(index, own, place, lane):
        send, recv = ga_send.at[index], ga_recv.at[index]
        sent = []

        def ship(src, dst, slot, peer):
            copy = remote(src, dst, send.at[slot], recv.at[slot], peer)
            copy.start()
            sent.append(copy)
            return copy

        line = {}
        mine = place(chip, lane)
        for s in order[::-1]:
            if s:
                line[s] = ship(own, mine, s, chip_at(shifted(s), spot) * 2 + core)

        plane = {}
        for s in order:
            if s:
                line[depth - s].wait_recv()
                source = chip_at(shifted(s), spot)
                view = place(source, lane)
                src = view
            else:
                source = chip
                view = mine
                src = own
            for c in range(PLANE - 1, 0, -1):
                plane[s, c] = ship(
                    src, view, depth + PLANE * s + c, chip_at(level, mirrored(c)) * 2 + core
                )
            plane[s, 0] = ship(src, view, (1 + PLANE) * depth + PLANE * s, partner)
        core_copies = [plane[s, 0] for s in order]
        for s in order:
            for c in (1, 2, 3):
                plane[s, c].wait_recv()
                source = chip_at(shifted(s), mirrored(c))
                view = place(source, lane)
                core_copies.append(
                    ship(view, view, (1 + PLANE) * depth + PLANE * s + c, partner)
                )
        for copy in core_copies:
            copy.wait_recv()
        return sent

    def whole_place(b):
        def place(which, lane):
            at = pl.multiple_of((which * 2 + lane) * cols, cols)
            return whole.at[b, :, pl.ds(at, cols)]

        return place

    def acts_place(b):
        def place(which, lane):
            at = pl.multiple_of(which * span, span)
            return acts.at[
                b, pl.ds(pl.multiple_of(lane * upper_rows, upper_rows), upper_rows), pl.ds(at, span)
            ]

        return place

    row_id = lax.broadcasted_iota(jnp.int32, (channels, states), 0) // GROUP_WIDTH
    col_id = lax.broadcasted_iota(jnp.int32, (channels, states), 1) // STATE_SIZE
    in_group = row_id == col_id
    lane_group = lax.broadcasted_iota(jnp.int32, (1, states), 1) // STATE_SIZE

    def spread(coefs):
        return jnp.where(in_group, jnp.concatenate([coefs] * groups, axis=0), 0.0)

    bars = []

    def prepare():
        for b in range(BLOCKS):
            step_size = jnp.zeros((1, states), f32)
            stepped = jnp.exp(log_step[b : b + 1, :])
            for g in range(groups):
                step_size = jnp.where(lane_group == g, stepped[:, g : g + 1], step_size)
            dr = decay_real[b : b + 1, :]
            di = decay_imag[b : b + 1, :]
            growth = jnp.exp(dr * step_size)
            angles = di * step_size
            bar_real = growth * jnp.cos(angles)
            bar_imag = growth * jnp.sin(angles)
            modulus = dr * dr + di * di
            minus = bar_real - 1.0
            hold_real = (minus * dr + bar_imag * di) / modulus
            hold_imag = (bar_imag * dr - minus * di) / modulus
            cr, ci = in_real[b], in_imag[b]
            push_w[b, :, :states] = spread(hold_real * cr - hold_imag * ci)
            push_w[b, :, states:] = spread(hold_real * ci + hold_imag * cr)
            read_w[b, :, :states] = spread(out_real[b])
            read_w[b, :, states:] = spread(-out_imag[b])
            bars.append((bar_real, bar_imag))

    sent = []
    stores = []
    whole[0, :, pl.ds(pl.multiple_of(me * cols, cols), cols)] = tokens[...]
    for b in range(BLOCKS):
        if b == 0:
            prepare()
            own = tokens
        else:
            own = current
            whole[b, :, pl.ds(pl.multiple_of(me * cols, cols), cols)] = current[...]
        sent += gather(2 * b, own, whole_place(b), core)

        gain = norm_gain[b : b + 1, :]
        bias = norm_bias[b : b + 1, :]

        @pl.loop(0, rows // 16)
        def _(r):
            at = pl.ds(pl.multiple_of(r * 16, 16), 16)
            wide = whole[b, at, :].astype(f32)
            center = jnp.mean(wide, axis=-1, keepdims=True)
            moved = wide - center
            var = jnp.mean(jnp.square(moved), axis=-1, keepdims=True)
            normed[at, :] = (moved * lax.rsqrt(var + norm_eps) * gain + bias).astype(bf16)

        loads[b][0].wait()
        drives = jnp.dot(normed[...], input_w[b], preferred_element_type=f32).astype(bf16)
        drives = drives.astype(f32)
        bar_real, bar_imag = bars[b]
        push = jnp.dot(drives, push_w[b], preferred_element_type=f32, precision=highest)
        loads[b][2].wait()
        loads[b][3].wait()
        old_real, old_imag = held_real[b], held_imag[b]
        fresh_real = bar_real * old_real - bar_imag * old_imag + push[:, :states]
        fresh_imag = bar_real * old_imag + bar_imag * old_real + push[:, states:]
        held_real[b] = fresh_real
        held_imag[b] = fresh_imag
        readout = lax.dot_general(
            jnp.concatenate([fresh_real, fresh_imag], axis=1),
            read_w[b],
            (((1,), (1,)), ((), ())),
            preferred_element_type=f32,
            precision=highest,
        )
        readout = readout + skip_coef[b : b + 1, :] * drives
        activated = jax.nn.gelu(readout).astype(bf16).astype(f32)
        left = jnp.where(core == 0, activated, 0.0)
        right = jnp.where(core == 0, 0.0, activated)
        half[b, 0] = jnp.concatenate([left, right], axis=1).astype(bf16)
        swap = remote(half.at[b, 0], half.at[b, 1], pair_send.at[b], pair_recv.at[b], partner)
        swap.start()
        for new, hbm, i in ((held_real, new_real_hbm, 0), (held_imag, new_imag_hbm, 1)):
            copy = pltpu.make_async_copy(new.at[b], hbm.at[b], store_sem.at[b, i])
            copy.start()
            stores.append(copy)
        loads[b][1].wait()
        gate = jnp.dot(normed[...], gate_w[b], preferred_element_type=f32).astype(bf16)
        gate = jax.nn.sigmoid(gate.astype(f32))
        swap.wait_recv()
        swap.wait_send()
        half[b, 2] = half[b, 0] + half[b, 1]
        mine_rows = pl.ds(pl.multiple_of(core * upper_rows, upper_rows), upper_rows)
        acts[b, mine_rows, pl.ds(pl.multiple_of(chip * span, span), span)] = half[
            b, 2, mine_rows, :
        ]
        sent += gather(2 * b + 1, half.at[b, 2, mine_rows, :], acts_place(b), core)

        loads[b][4].wait()
        loads[b][5].wait()
        values = jnp.dot(acts[b], value_w[b], preferred_element_type=f32).astype(bf16)
        gating = jnp.dot(acts[b], gating_w[b], preferred_element_type=f32).astype(bf16)
        mixture = (gate * values.astype(f32) * jax.nn.sigmoid(gating.astype(f32))).astype(bf16)

        loads[b][6].wait()
        lots = PLANE * cols
        to_core = {}
        send, recv = rs_send.at[b], rs_recv.at[b]
        steps = list(range(1, depth)) + [0]
        for s in steps:
            lev = shifted(s)
            sums = jnp.dot(
                mixture,
                output_w[b, :, pl.ds(pl.multiple_of(lev * 2 * lots, 2 * lots), 2 * lots)],
                preferred_element_type=f32,
            ).astype(bf16)
            for k in range(PLANE):
                for lane in range(2):
                    partial_sums[b, lane, s, k] = sums[
                        :, (2 * k + lane) * cols : (2 * k + lane + 1) * cols
                    ]
            to_core[s] = remote(
                partial_sums.at[b, 1 - core, s],
                from_core.at[b, s],
                send.at[s],
                recv.at[s],
                partner,
            )
            to_core[s].start()
            sent.append(to_core[s])
        to_plane = {}
        for s in steps:
            to_core[s].wait_recv()
            merged[b, s] = (
                partial_sums[b, core, s].astype(f32) + from_core[b, s].astype(f32)
            ).astype(bf16)
            for c in (3, 2, 1):
                slot = depth + PLANE * s + c
                to_plane[s, c] = remote(
                    merged.at[b, s, mirrored(c)],
                    from_plane.at[b, s, c],
                    send.at[slot],
                    recv.at[slot],
                    chip_at(level, mirrored(c)) * 2 + core,
                )
                to_plane[s, c].start()
                sent.append(to_plane[s, c])
        to_line = {}
        for s in steps:
            total = merged[b, s, spot].astype(f32)
            for c in (3, 2, 1):
                to_plane[s, c].wait_recv()
                total = total + from_plane[b, s, c].astype(f32)
            if s:
                upper[b, s] = total.astype(bf16)
                slot = depth + PLANE * depth + s
                to_line[s] = remote(
                    upper.at[b, s],
                    from_line.at[b, s],
                    send.at[slot],
                    recv.at[slot],
                    chip_at(shifted(s), spot) * 2 + core,
                )
                to_line[s].start()
                sent.append(to_line[s])
        for s in range(1, depth):
            to_line[s].wait_recv()
            total = total + from_line[b, s].astype(f32)
        if b + 1 < BLOCKS:
            current[...] = total.astype(bf16)
        else:
            block_output[...] = total.astype(bf16)
    for copy in sent:
        copy.wait_send()
    for copy in stores:
        copy.wait()


def shards(
    tokens,
    norm_gain,
    norm_bias,
    input_weight,
    gate_weight,
    decay_real,
    decay_imag,
    log_step,
    input_coef_real,
    input_coef_imag,
    output_coef_real,
    output_coef_imag,
    skip_coef,
    value_weight,
    gating_weight,
    output_weight,
    state_real,
    state_imag,
    devices,
):
    depth = devices // (2 * PLANE)
    rows, cols = tokens.shape
    channels = skip_coef.shape[1]
    states = decay_real.shape[1]
    if cols % 128 or (2 * channels) % 128 or devices % (2 * PLANE):
        return plain_shards(
            tokens,
            norm_gain,
            norm_bias,
            input_weight,
            gate_weight,
            decay_real,
            decay_imag,
            log_step,
            input_coef_real,
            input_coef_imag,
            output_coef_real,
            output_coef_imag,
            skip_coef,
            value_weight,
            gating_weight,
            output_weight,
            state_real,
            state_imag,
        )
    width = cols * devices
    ssm = channels * devices
    turned = [
        jnp.swapaxes(a, 1, 2)
        for a in (input_coef_real, input_coef_imag, output_coef_real, output_coef_imag)
    ]
    vmem = pl.BlockSpec(memory_space=pltpu.VMEM)
    hbm = pl.BlockSpec(memory_space=pl.ANY)
    dma = pltpu.SemaphoreType.DMA
    gather_slots = (1 + 2 * PLANE) * depth
    scatter_slots = (2 + PLANE) * depth
    lot = (depth, PLANE, rows, cols)
    return pl.pallas_call(
        partial(kernel, depth),
        out_shape=(
            jax.ShapeDtypeStruct((rows, cols), bf16),
            jax.ShapeDtypeStruct(state_real.shape, f32),
            jax.ShapeDtypeStruct(state_imag.shape, f32),
        ),
        in_specs=[vmem] * 11 + [hbm] * 7,
        out_specs=(vmem, hbm, hbm),
        scratch_shapes=[
            pltpu.VMEM(input_weight.shape, bf16),
            pltpu.VMEM(gate_weight.shape, bf16),
            pltpu.VMEM(value_weight.shape, bf16),
            pltpu.VMEM(gating_weight.shape, bf16),
            pltpu.VMEM(output_weight.shape, bf16),
            pltpu.VMEM(state_real.shape, f32),
            pltpu.VMEM(state_imag.shape, f32),
            pltpu.VMEM((BLOCKS, rows, width), bf16),
            pltpu.VMEM((rows, width), bf16),
            pltpu.VMEM((rows, cols), bf16),
            pltpu.VMEM((BLOCKS, 3, rows, 2 * channels), bf16),
            pltpu.VMEM((BLOCKS, rows, ssm), bf16),
            pltpu.VMEM((BLOCKS, channels, 2 * states), f32),
            pltpu.VMEM((BLOCKS, channels, 2 * states), f32),
            pltpu.VMEM((BLOCKS, 2) + lot, bf16),
            pltpu.VMEM((BLOCKS,) + lot, bf16),
            pltpu.VMEM((BLOCKS,) + lot, bf16),
            pltpu.VMEM((BLOCKS,) + lot, bf16),
            pltpu.VMEM((BLOCKS, depth, rows, cols), bf16),
            pltpu.VMEM((BLOCKS, depth, rows, cols), bf16),
            dma((BLOCKS, 7)),
            dma((BLOCKS, 2)),
            dma((BLOCKS,)),
            dma((BLOCKS,)),
            dma((2 * BLOCKS, gather_slots)),
            dma((2 * BLOCKS, gather_slots)),
            dma((BLOCKS, scatter_slots)),
            dma((BLOCKS, scatter_slots)),
        ],
        compiler_params=pltpu.CompilerParams(
            collective_id=0, has_side_effects=True, vmem_limit_bytes=60 * 1024 * 1024
        ),
    )(
        tokens,
        norm_gain,
        norm_bias,
        decay_real,
        decay_imag,
        log_step,
        *turned,
        skip_coef,
        input_weight,
        gate_weight,
        value_weight,
        gating_weight,
        output_weight,
        state_real,
        state_imag,
    )


def folded(shard, axis, dim, absorb, state):
    everything = jax.tree.map(lambda a: lax.all_gather(a, axis, axis=dim, tiled=True), shard)
    return absorb(state, everything, jnp.int32(0))


def layer_norm(values, scales, offsets):
    widened = values.astype(jnp.float32)
    center = jnp.mean(widened, axis=-1, keepdims=True)
    spread = jnp.mean(jnp.square(widened - center), axis=-1, keepdims=True)
    normed = (widened - center) * lax.rsqrt(spread + norm_eps) * scales + offsets
    return normed.astype(jnp.bfloat16)


def discretize(decay_real, decay_imag, step_size, coef_real, coef_imag):
    growth = jnp.exp(decay_real * step_size)
    angles = decay_imag * step_size
    bar_real = growth * jnp.cos(angles)
    bar_imag = growth * jnp.sin(angles)
    modulus = decay_real * decay_real + decay_imag * decay_imag
    minus_real = bar_real - 1.0
    hold_real = (minus_real * decay_real + bar_imag * decay_imag) / modulus
    hold_imag = (bar_imag * decay_real - minus_real * decay_imag) / modulus
    coupling_real = hold_real[:, None] * coef_real - hold_imag[:, None] * coef_imag
    coupling_imag = hold_real[:, None] * coef_imag + hold_imag[:, None] * coef_real
    return (bar_real, bar_imag, coupling_real, coupling_imag)


def fold_pair(first_weight, second_weight, totals, piece, start):
    first_rows = lax.dynamic_slice_in_dim(first_weight, start, piece.shape[1], 0)
    second_rows = lax.dynamic_slice_in_dim(second_weight, start, piece.shape[1], 0)
    return (
        totals[0] + jnp.dot(piece, first_rows, preferred_element_type=jnp.float32),
        totals[1] + jnp.dot(piece, second_rows, preferred_element_type=jnp.float32),
    )


def fold_single(weights, total, piece, start):
    rows = lax.dynamic_slice_in_dim(weights, start, piece.shape[1], 0)
    return total + jnp.dot(piece, rows, preferred_element_type=jnp.float32)


def plain_shards(
    tokens,
    norm_gain,
    norm_bias,
    input_weight,
    gate_weight,
    decay_real,
    decay_imag,
    log_step,
    input_coef_real,
    input_coef_imag,
    output_coef_real,
    output_coef_imag,
    skip_coef,
    value_weight,
    gating_weight,
    output_weight,
    state_real,
    state_imag,
):
    channels = skip_coef.shape[1]
    local_groups = channels // GROUP_WIDTH
    model_cols = gate_weight.shape[2]
    batch_rows = tokens.shape[0]
    turned = lax.all_to_all(output_weight, "tp", split_axis=2, concat_axis=1, tiled=True)
    current = tokens
    new_reals = []
    new_imags = []
    for block_index in range(BLOCKS):
        whole = lax.all_gather(current, "tp", axis=1, tiled=True)
        normed = layer_norm(whole, norm_gain[block_index], norm_bias[block_index])
        drives = jnp.dot(
            normed, input_weight[block_index], preferred_element_type=jnp.float32
        ).astype(jnp.bfloat16)
        gate_rows = jnp.dot(
            normed, gate_weight[block_index], preferred_element_type=jnp.float32
        ).astype(jnp.bfloat16)
        step_size = jnp.repeat(jnp.exp(log_step[block_index]), STATE_SIZE)
        bar_real, bar_imag, coupling_real, coupling_imag = discretize(
            decay_real[block_index],
            decay_imag[block_index],
            step_size,
            input_coef_real[block_index],
            input_coef_imag[block_index],
        )
        grouped = drives.astype(jnp.float32).reshape(batch_rows, local_groups, GROUP_WIDTH)
        push_real = jnp.einsum(
            "bgc,gpc->bgp",
            grouped,
            coupling_real.reshape(local_groups, STATE_SIZE, GROUP_WIDTH),
            precision=highest,
        ).reshape(batch_rows, local_groups * STATE_SIZE)
        push_imag = jnp.einsum(
            "bgc,gpc->bgp",
            grouped,
            coupling_imag.reshape(local_groups, STATE_SIZE, GROUP_WIDTH),
            precision=highest,
        ).reshape(batch_rows, local_groups * STATE_SIZE)
        old_real = state_real[block_index]
        old_imag = state_imag[block_index]
        fresh_real = bar_real * old_real - bar_imag * old_imag + push_real
        fresh_imag = bar_real * old_imag + bar_imag * old_real + push_imag
        readout = jnp.einsum(
            "bgp,gpc->bgc",
            fresh_real.reshape(batch_rows, local_groups, STATE_SIZE),
            output_coef_real[block_index].reshape(local_groups, STATE_SIZE, GROUP_WIDTH),
            precision=highest,
        )
        readout = readout - jnp.einsum(
            "bgp,gpc->bgc",
            fresh_imag.reshape(batch_rows, local_groups, STATE_SIZE),
            output_coef_imag[block_index].reshape(local_groups, STATE_SIZE, GROUP_WIDTH),
            precision=highest,
        )
        readout = readout.reshape(batch_rows, channels) + skip_coef[block_index] * drives.astype(
            jnp.float32
        )
        new_reals.append(fresh_real)
        new_imags.append(fresh_imag)
        activated = jax.nn.gelu(readout).astype(jnp.bfloat16)
        empty_cols = jnp.zeros((batch_rows, model_cols), jnp.float32)
        value_sums, gating_sums = folded(
            activated,
            "tp",
            1,
            partial(fold_pair, value_weight[block_index], gating_weight[block_index]),
            (empty_cols, empty_cols),
        )
        values = value_sums.astype(jnp.bfloat16)
        gating = gating_sums.astype(jnp.bfloat16)
        mixture = (
            jax.nn.sigmoid(gate_rows.astype(jnp.float32))
            * values.astype(jnp.float32)
            * jax.nn.sigmoid(gating.astype(jnp.float32))
        ).astype(jnp.bfloat16)
        summed = folded(mixture, "tp", 1, partial(fold_single, turned[block_index]), empty_cols)
        current = summed.astype(jnp.bfloat16)
    return (current, jnp.stack(new_reals), jnp.stack(new_imags))


def solution(mesh):
    return jax.shard_map(
        partial(shards, devices=mesh.shape["tp"]),
        mesh=mesh,
        in_specs=(
            P(None, "tp"),
            P(),
            P(),
            P(None, None, "tp"),
            P(None, None, "tp"),
            P(None, "tp"),
            P(None, "tp"),
            P(None, "tp"),
            P(None, "tp", None),
            P(None, "tp", None),
            P(None, "tp", None),
            P(None, "tp", None),
            P(None, "tp"),
            P(None, None, "tp"),
            P(None, None, "tp"),
            P(None, "tp", None),
            P(None, None, "tp"),
            P(None, None, "tp"),
        ),
        out_specs=(P(None, "tp"), P(None, None, "tp"), P(None, None, "tp")),
        check_vma=False,
    )
```

```python
from functools import partial

import jax
import jax.numpy as jnp
from jax import lax
from jax.experimental import pallas as pl
from jax.experimental.pallas import tpu as pltpu
from jax.sharding import PartitionSpec as P

GROUP_WIDTH = 16
STATE_SIZE = 64
BLOCKS = 2
PLANE = 4

norm_eps = 1e-05
highest = lax.Precision.HIGHEST
f32 = jnp.float32
bf16 = jnp.bfloat16


def kernel(
    depth,
    tokens,
    norm_gain,
    norm_bias,
    decay_real,
    decay_imag,
    log_step,
    in_real,
    in_imag,
    out_real,
    out_imag,
    skip_coef,
    input_hbm,
    gate_hbm,
    value_hbm,
    gating_hbm,
    output_hbm,
    state_real_hbm,
    state_imag_hbm,
    block_output,
    new_real_hbm,
    new_imag_hbm,
    input_w,
    gate_w,
    linear_w,
    output_w,
    held_real,
    held_imag,
    whole,
    normed,
    current,
    half,
    acts,
    push_w,
    read_w,
    partial_sums,
    from_core,
    merged,
    from_plane,
    upper,
    from_line,
    load_sem,
    store_sem,
    pair_send,
    pair_recv,
    ga_send,
    ga_recv,
    rs_send,
    rs_recv,
):
    rows, cols = tokens.shape
    channels = skip_coef.shape[1]
    states = decay_real.shape[1]
    groups = channels // GROUP_WIDTH
    span = 2 * channels
    upper_rows = rows // 2

    me = lax.axis_index("tp")
    core = lax.rem(me, 2)
    chip = me // 2
    spot = lax.rem(chip, PLANE)
    level = chip // PLANE
    partner = chip * 2 + (1 - core)

    def chip_at(lev, place):
        return lev * PLANE + place

    def shifted(step):
        return lax.rem(level + step, depth)

    def mirrored(code):
        if code == 0:
            return spot
        x, y = lax.rem(spot, 2), spot // 2
        if code & 1:
            x = 1 - x
        if code & 2:
            y = 1 - y
        return y * 2 + x

    line_peers = [chip_at(shifted(s), spot) * 2 + core for s in range(1, depth)]
    plane_peers = [chip_at(level, mirrored(c)) * 2 + core for c in range(1, PLANE)]

    loads = []
    weights = (
        (input_hbm, input_w),
        (gate_hbm, gate_w),
        (state_real_hbm, held_real),
        (state_imag_hbm, held_imag),
        (value_hbm, linear_w.at[:, :, pl.ds(0, cols)]),
        (gating_hbm, linear_w.at[:, :, pl.ds(cols, cols)]),
        (output_hbm, output_w),
    )
    for b in range(BLOCKS):
        block_loads = []
        for i, (src, dst) in enumerate(weights):
            copy = pltpu.make_async_copy(src.at[b], dst.at[b], load_sem.at[b, i])
            copy.start()
            block_loads.append(copy)
        loads.append(block_loads)

    barrier = pltpu.get_barrier_semaphore()
    everyone = line_peers + plane_peers + [partner]
    for peer in everyone:
        pl.semaphore_signal(
            barrier, inc=1, device_id=(peer,), device_id_type=pl.DeviceIdType.MESH
        )
    pl.semaphore_wait(barrier, len(everyone))

    def remote(src, dst, send, recv, peer):
        return pltpu.make_async_remote_copy(
            src_ref=src,
            dst_ref=dst,
            send_sem=send,
            recv_sem=recv,
            device_id=(peer,),
            device_id_type=pl.DeviceIdType.MESH,
        )

    order = sorted(range(depth), key=lambda s: min(s, depth - s))

    def gather(index, own, place, lane, during):
        send, recv = ga_send.at[index], ga_recv.at[index]
        sent = []

        def ship(src, dst, slot, peer):
            copy = remote(src, dst, send.at[slot], recv.at[slot], peer)
            copy.start()
            sent.append(copy)
            return copy

        line = {}
        mine = place(chip, lane)
        for s in order[::-1]:
            if s:
                line[s] = ship(own, mine, s, chip_at(shifted(s), spot) * 2 + core)

        plane = {}
        for s in order:
            if s == order[1]:
                during()
            if s:
                line[depth - s].wait_recv()
                source = chip_at(shifted(s), spot)
                view = place(source, lane)
                src = view
            else:
                source = chip
                view = mine
                src = own
            for c in range(PLANE - 1, 0, -1):
                plane[s, c] = ship(
                    src, view, depth + PLANE * s + c, chip_at(level, mirrored(c)) * 2 + core
                )
            plane[s, 0] = ship(src, view, (1 + PLANE) * depth + PLANE * s, partner)
        core_copies = [plane[s, 0] for s in order]
        for s in order:
            for c in (1, 2, 3):
                plane[s, c].wait_recv()
                source = chip_at(shifted(s), mirrored(c))
                view = place(source, lane)
                core_copies.append(
                    ship(view, view, (1 + PLANE) * depth + PLANE * s + c, partner)
                )
        for copy in core_copies:
            copy.wait_recv()
        return sent

    def whole_place(b):
        def place(which, lane):
            at = pl.multiple_of((which * 2 + lane) * cols, cols)
            return whole.at[b, :, pl.ds(at, cols)]

        return place

    def acts_place(b):
        def place(which, lane):
            at = pl.multiple_of(which * span, span)
            return acts.at[
                b, pl.ds(pl.multiple_of(lane * upper_rows, upper_rows), upper_rows), pl.ds(at, span)
            ]

        return place

    row_id = lax.broadcasted_iota(jnp.int32, (channels, states), 0) // GROUP_WIDTH
    col_id = lax.broadcasted_iota(jnp.int32, (channels, states), 1) // STATE_SIZE
    in_group = row_id == col_id
    lane_group = lax.broadcasted_iota(jnp.int32, (1, states), 1) // STATE_SIZE

    def spread(coefs):
        return jnp.where(in_group, jnp.concatenate([coefs] * groups, axis=0), 0.0)

    bars = []

    def prepare(b):
        if True:
            step_size = jnp.zeros((1, states), f32)
            stepped = jnp.exp(log_step[b : b + 1, :])
            for g in range(groups):
                step_size = jnp.where(lane_group == g, stepped[:, g : g + 1], step_size)
            dr = decay_real[b : b + 1, :]
            di = decay_imag[b : b + 1, :]
            growth = jnp.exp(dr * step_size)
            angles = di * step_size
            bar_real = growth * jnp.cos(angles)
            bar_imag = growth * jnp.sin(angles)
            modulus = dr * dr + di * di
            minus = bar_real - 1.0
            hold_real = (minus * dr + bar_imag * di) / modulus
            hold_imag = (bar_imag * dr - minus * di) / modulus
            cr, ci = in_real[b], in_imag[b]
            push_w[b, :, :states] = spread(hold_real * cr - hold_imag * ci)
            push_w[b, :, states:] = spread(hold_real * ci + hold_imag * cr)
            read_w[b, :, :states] = spread(out_real[b])
            read_w[b, :, states:] = spread(-out_imag[b])
            bars.append((bar_real, bar_imag))

    sent = []
    stores = []
    whole[0, :, pl.ds(pl.multiple_of(me * cols, cols), cols)] = tokens[...]
    for b in range(BLOCKS):
        if b == 0:
            own = tokens
        else:
            own = current
            whole[b, :, pl.ds(pl.multiple_of(me * cols, cols), cols)] = current[...]
        sent += gather(2 * b, own, whole_place(b), core, partial(prepare, b))

        gain = norm_gain[b : b + 1, :]
        bias = norm_bias[b : b + 1, :]

        @pl.loop(0, rows // 16, unroll=8)
        def _(r):
            at = pl.ds(pl.multiple_of(r * 16, 16), 16)
            wide = whole[b, at, :].astype(f32)
            center = jnp.mean(wide, axis=-1, keepdims=True)
            moved = wide - center
            var = jnp.mean(jnp.square(moved), axis=-1, keepdims=True)
            normed[at, :] = (moved * lax.rsqrt(var + norm_eps) * gain + bias).astype(bf16)

        loads[b][0].wait()
        drives = lax.dot_general(
            normed[...], input_w[b], (((1,), (1,)), ((), ())), preferred_element_type=f32
        ).astype(bf16)
        drives = drives.astype(f32)
        bar_real, bar_imag = bars[b]
        push = jnp.dot(drives, push_w[b], preferred_element_type=f32)
        loads[b][2].wait()
        loads[b][3].wait()
        old_real, old_imag = held_real[b], held_imag[b]
        fresh_real = bar_real * old_real - bar_imag * old_imag + push[:, :states]
        fresh_imag = bar_real * old_imag + bar_imag * old_real + push[:, states:]
        held_real[b] = fresh_real
        held_imag[b] = fresh_imag
        readout = lax.dot_general(
            jnp.concatenate([fresh_real, fresh_imag], axis=1),
            read_w[b],
            (((1,), (1,)), ((), ())),
            preferred_element_type=f32,
        )
        readout = readout + skip_coef[b : b + 1, :] * drives
        activated = jax.nn.gelu(readout).astype(bf16).astype(f32)
        left = jnp.where(core == 0, activated, 0.0)
        right = jnp.where(core == 0, 0.0, activated)
        half[b, 0] = jnp.concatenate([left, right], axis=1).astype(bf16)
        swap = remote(half.at[b, 0], half.at[b, 1], pair_send.at[b], pair_recv.at[b], partner)
        swap.start()
        for new, hbm, i in ((held_real, new_real_hbm, 0), (held_imag, new_imag_hbm, 1)):
            copy = pltpu.make_async_copy(new.at[b], hbm.at[b], store_sem.at[b, i])
            copy.start()
            stores.append(copy)
        gates = []

        def open_gate():
            loads[b][1].wait()
            gate = jnp.dot(normed[...], gate_w[b], preferred_element_type=f32).astype(bf16)
            gates.append(jax.nn.sigmoid(gate.astype(f32)))

        swap.wait_recv()
        swap.wait_send()
        half[b, 2] = half[b, 0] + half[b, 1]
        mine_rows = pl.ds(pl.multiple_of(core * upper_rows, upper_rows), upper_rows)
        acts[b, mine_rows, pl.ds(pl.multiple_of(chip * span, span), span)] = half[
            b, 2, mine_rows, :
        ]
        sent += gather(2 * b + 1, half.at[b, 2, mine_rows, :], acts_place(b), core, open_gate)

        loads[b][4].wait()
        loads[b][5].wait()
        both = jnp.dot(acts[b], linear_w[b], preferred_element_type=f32).astype(bf16)
        values, gating = both[:, :cols], both[:, cols:]
        mixture = (gates[0] * values.astype(f32) * jax.nn.sigmoid(gating.astype(f32))).astype(bf16)

        loads[b][6].wait()
        lots = PLANE * cols
        to_core = {}
        to_plane = {}
        send, recv = rs_send.at[b], rs_recv.at[b]
        steps = list(range(1, depth)) + [0]

        def merge(s):
            to_core[s].wait_recv()
            merged[b, s] = (
                partial_sums[b, core, s].astype(f32) + from_core[b, s].astype(f32)
            ).astype(bf16)
            for c in (3, 2, 1):
                slot = depth + PLANE * s + c
                to_plane[s, c] = remote(
                    merged.at[b, s, mirrored(c)],
                    from_plane.at[b, s, c],
                    send.at[slot],
                    recv.at[slot],
                    chip_at(level, mirrored(c)) * 2 + core,
                )
                to_plane[s, c].start()
                sent.append(to_plane[s, c])

        for at, s in enumerate(steps):
            lev = shifted(s)
            sums = jnp.dot(
                mixture,
                output_w[b, :, pl.ds(pl.multiple_of(lev * 2 * lots, 2 * lots), 2 * lots)],
                preferred_element_type=f32,
            ).astype(bf16)
            for k in range(PLANE):
                for lane in range(2):
                    partial_sums[b, lane, s, k] = sums[
                        :, (2 * k + lane) * cols : (2 * k + lane + 1) * cols
                    ]
            to_core[s] = remote(
                partial_sums.at[b, 1 - core, s],
                from_core.at[b, s],
                send.at[s],
                recv.at[s],
                partner,
            )
            to_core[s].start()
            sent.append(to_core[s])
            if at >= 2:
                merge(steps[at - 2])
        for s in steps[-2:]:
            merge(s)
        to_line = {}
        for s in steps:
            total = merged[b, s, spot].astype(f32)
            for c in (3, 2, 1):
                to_plane[s, c].wait_recv()
                total = total + from_plane[b, s, c].astype(f32)
            if s:
                upper[b, s] = total.astype(bf16)
                slot = depth + PLANE * depth + s
                to_line[s] = remote(
                    upper.at[b, s],
                    from_line.at[b, s],
                    send.at[slot],
                    recv.at[slot],
                    chip_at(shifted(s), spot) * 2 + core,
                )
                to_line[s].start()
                sent.append(to_line[s])
        for s in range(1, depth):
            to_line[s].wait_recv()
            total = total + from_line[b, s].astype(f32)
        if b + 1 < BLOCKS:
            current[...] = total.astype(bf16)
        else:
            block_output[...] = total.astype(bf16)
    for copy in sent:
        copy.wait_send()
    for copy in stores:
        copy.wait()


def hand_over(*refs):
    sources, targets, held = refs[:3], refs[3:6], refs[6:9]
    load_sem, store_sem = refs[9:]
    loads = [pltpu.make_async_copy(a, h, load_sem.at[i]) for i, (a, h) in enumerate(zip(sources, held))]
    for copy in loads:
        copy.start()
    stores = []
    for i, (h, t) in enumerate(zip(held, targets)):
        loads[i].wait()
        copy = pltpu.make_async_copy(h, t, store_sem.at[i])
        copy.start()
        stores.append(copy)
    for copy in stores:
        copy.wait()


def shards(
    tokens,
    norm_gain,
    norm_bias,
    input_weight,
    gate_weight,
    decay_real,
    decay_imag,
    log_step,
    input_coef_real,
    input_coef_imag,
    output_coef_real,
    output_coef_imag,
    skip_coef,
    value_weight,
    gating_weight,
    output_weight,
    state_real,
    state_imag,
    devices,
):
    depth = devices // (2 * PLANE)
    rows, cols = tokens.shape
    channels = skip_coef.shape[1]
    states = decay_real.shape[1]
    if cols % 128 or (2 * channels) % 128 or devices % (2 * PLANE):
        return plain_shards(
            tokens,
            norm_gain,
            norm_bias,
            input_weight,
            gate_weight,
            decay_real,
            decay_imag,
            log_step,
            input_coef_real,
            input_coef_imag,
            output_coef_real,
            output_coef_imag,
            skip_coef,
            value_weight,
            gating_weight,
            output_weight,
            state_real,
            state_imag,
        )
    width = cols * devices
    input_turned = jnp.swapaxes(input_weight, 1, 2)
    ssm = channels * devices
    turned = [
        jnp.swapaxes(a, 1, 2)
        for a in (input_coef_real, input_coef_imag, output_coef_real, output_coef_imag)
    ]
    vmem = pl.BlockSpec(memory_space=pltpu.VMEM)
    hbm = pl.BlockSpec(memory_space=pl.ANY)
    dma = pltpu.SemaphoreType.DMA
    gather_slots = (1 + 2 * PLANE) * depth
    scatter_slots = (2 + PLANE) * depth
    lot = (depth, PLANE, rows, cols)
    outs = pl.pallas_call(
        partial(kernel, depth),
        out_shape=(
            jax.ShapeDtypeStruct((rows, cols), bf16),
            jax.ShapeDtypeStruct(state_real.shape, f32),
            jax.ShapeDtypeStruct(state_imag.shape, f32),
        ),
        in_specs=[vmem] * 11 + [hbm] * 7,
        out_specs=(vmem, hbm, hbm),
        scratch_shapes=[
            pltpu.VMEM(input_turned.shape, bf16),
            pltpu.VMEM(gate_weight.shape, bf16),
            pltpu.VMEM((BLOCKS, ssm, 2 * cols), bf16),
            pltpu.VMEM(output_weight.shape, bf16),
            pltpu.VMEM(state_real.shape, f32),
            pltpu.VMEM(state_imag.shape, f32),
            pltpu.VMEM((BLOCKS, rows, width), bf16),
            pltpu.VMEM((rows, width), bf16),
            pltpu.VMEM((rows, cols), bf16),
            pltpu.VMEM((BLOCKS, 3, rows, 2 * channels), bf16),
            pltpu.VMEM((BLOCKS, rows, ssm), bf16),
            pltpu.VMEM((BLOCKS, channels, 2 * states), f32),
            pltpu.VMEM((BLOCKS, channels, 2 * states), f32),
            pltpu.VMEM((BLOCKS, 2) + lot, bf16),
            pltpu.VMEM((BLOCKS,) + lot, bf16),
            pltpu.VMEM((BLOCKS,) + lot, bf16),
            pltpu.VMEM((BLOCKS,) + lot, bf16),
            pltpu.VMEM((BLOCKS, depth, rows, cols), bf16),
            pltpu.VMEM((BLOCKS, depth, rows, cols), bf16),
            dma((BLOCKS, 7)),
            dma((BLOCKS, 2)),
            dma((BLOCKS,)),
            dma((BLOCKS,)),
            dma((2 * BLOCKS, gather_slots)),
            dma((2 * BLOCKS, gather_slots)),
            dma((BLOCKS, scatter_slots)),
            dma((BLOCKS, scatter_slots)),
        ],
        compiler_params=pltpu.CompilerParams(
            collective_id=0, has_side_effects=True, vmem_limit_bytes=60 * 1024 * 1024
        ),
    )(
        tokens,
        norm_gain,
        norm_bias,
        decay_real,
        decay_imag,
        log_step,
        *turned,
        skip_coef,
        input_turned,
        gate_weight,
        value_weight,
        gating_weight,
        output_weight,
        state_real,
        state_imag,
    )
    return pl.pallas_call(
        hand_over,
        out_shape=tuple(jax.ShapeDtypeStruct(o.shape, o.dtype) for o in outs),
        in_specs=[hbm] * 3,
        out_specs=(hbm,) * 3,
        scratch_shapes=[pltpu.VMEM(o.shape, o.dtype) for o in outs] + [dma((3,)), dma((3,))],
    )(*outs)


def folded(shard, axis, dim, absorb, state):
    everything = jax.tree.map(lambda a: lax.all_gather(a, axis, axis=dim, tiled=True), shard)
    return absorb(state, everything, jnp.int32(0))


def layer_norm(values, scales, offsets):
    widened = values.astype(jnp.float32)
    center = jnp.mean(widened, axis=-1, keepdims=True)
    spread = jnp.mean(jnp.square(widened - center), axis=-1, keepdims=True)
    normed = (widened - center) * lax.rsqrt(spread + norm_eps) * scales + offsets
    return normed.astype(jnp.bfloat16)


def discretize(decay_real, decay_imag, step_size, coef_real, coef_imag):
    growth = jnp.exp(decay_real * step_size)
    angles = decay_imag * step_size
    bar_real = growth * jnp.cos(angles)
    bar_imag = growth * jnp.sin(angles)
    modulus = decay_real * decay_real + decay_imag * decay_imag
    minus_real = bar_real - 1.0
    hold_real = (minus_real * decay_real + bar_imag * decay_imag) / modulus
    hold_imag = (bar_imag * decay_real - minus_real * decay_imag) / modulus
    coupling_real = hold_real[:, None] * coef_real - hold_imag[:, None] * coef_imag
    coupling_imag = hold_real[:, None] * coef_imag + hold_imag[:, None] * coef_real
    return (bar_real, bar_imag, coupling_real, coupling_imag)


def fold_pair(first_weight, second_weight, totals, piece, start):
    first_rows = lax.dynamic_slice_in_dim(first_weight, start, piece.shape[1], 0)
    second_rows = lax.dynamic_slice_in_dim(second_weight, start, piece.shape[1], 0)
    return (
        totals[0] + jnp.dot(piece, first_rows, preferred_element_type=jnp.float32),
        totals[1] + jnp.dot(piece, second_rows, preferred_element_type=jnp.float32),
    )


def fold_single(weights, total, piece, start):
    rows = lax.dynamic_slice_in_dim(weights, start, piece.shape[1], 0)
    return total + jnp.dot(piece, rows, preferred_element_type=jnp.float32)


def plain_shards(
    tokens,
    norm_gain,
    norm_bias,
    input_weight,
    gate_weight,
    decay_real,
    decay_imag,
    log_step,
    input_coef_real,
    input_coef_imag,
    output_coef_real,
    output_coef_imag,
    skip_coef,
    value_weight,
    gating_weight,
    output_weight,
    state_real,
    state_imag,
):
    channels = skip_coef.shape[1]
    local_groups = channels // GROUP_WIDTH
    model_cols = gate_weight.shape[2]
    batch_rows = tokens.shape[0]
    turned = lax.all_to_all(output_weight, "tp", split_axis=2, concat_axis=1, tiled=True)
    current = tokens
    new_reals = []
    new_imags = []
    for block_index in range(BLOCKS):
        whole = lax.all_gather(current, "tp", axis=1, tiled=True)
        normed = layer_norm(whole, norm_gain[block_index], norm_bias[block_index])
        drives = jnp.dot(
            normed, input_weight[block_index], preferred_element_type=jnp.float32
        ).astype(jnp.bfloat16)
        gate_rows = jnp.dot(
            normed, gate_weight[block_index], preferred_element_type=jnp.float32
        ).astype(jnp.bfloat16)
        step_size = jnp.repeat(jnp.exp(log_step[block_index]), STATE_SIZE)
        bar_real, bar_imag, coupling_real, coupling_imag = discretize(
            decay_real[block_index],
            decay_imag[block_index],
            step_size,
            input_coef_real[block_index],
            input_coef_imag[block_index],
        )
        grouped = drives.astype(jnp.float32).reshape(batch_rows, local_groups, GROUP_WIDTH)
        push_real = jnp.einsum(
            "bgc,gpc->bgp",
            grouped,
            coupling_real.reshape(local_groups, STATE_SIZE, GROUP_WIDTH),
            precision=highest,
        ).reshape(batch_rows, local_groups * STATE_SIZE)
        push_imag = jnp.einsum(
            "bgc,gpc->bgp",
            grouped,
            coupling_imag.reshape(local_groups, STATE_SIZE, GROUP_WIDTH),
            precision=highest,
        ).reshape(batch_rows, local_groups * STATE_SIZE)
        old_real = state_real[block_index]
        old_imag = state_imag[block_index]
        fresh_real = bar_real * old_real - bar_imag * old_imag + push_real
        fresh_imag = bar_real * old_imag + bar_imag * old_real + push_imag
        readout = jnp.einsum(
            "bgp,gpc->bgc",
            fresh_real.reshape(batch_rows, local_groups, STATE_SIZE),
            output_coef_real[block_index].reshape(local_groups, STATE_SIZE, GROUP_WIDTH),
            precision=highest,
        )
        readout = readout - jnp.einsum(
            "bgp,gpc->bgc",
            fresh_imag.reshape(batch_rows, local_groups, STATE_SIZE),
            output_coef_imag[block_index].reshape(local_groups, STATE_SIZE, GROUP_WIDTH),
            precision=highest,
        )
        readout = readout.reshape(batch_rows, channels) + skip_coef[block_index] * drives.astype(
            jnp.float32
        )
        new_reals.append(fresh_real)
        new_imags.append(fresh_imag)
        activated = jax.nn.gelu(readout).astype(jnp.bfloat16)
        empty_cols = jnp.zeros((batch_rows, model_cols), jnp.float32)
        value_sums, gating_sums = folded(
            activated,
            "tp",
            1,
            partial(fold_pair, value_weight[block_index], gating_weight[block_index]),
            (empty_cols, empty_cols),
        )
        values = value_sums.astype(jnp.bfloat16)
        gating = gating_sums.astype(jnp.bfloat16)
        mixture = (
            jax.nn.sigmoid(gate_rows.astype(jnp.float32))
            * values.astype(jnp.float32)
            * jax.nn.sigmoid(gating.astype(jnp.float32))
        ).astype(jnp.bfloat16)
        summed = folded(mixture, "tp", 1, partial(fold_single, turned[block_index]), empty_cols)
        current = summed.astype(jnp.bfloat16)
    return (current, jnp.stack(new_reals), jnp.stack(new_imags))


def solution(mesh):
    return jax.shard_map(
        partial(shards, devices=mesh.shape["tp"]),
        mesh=mesh,
        in_specs=(
            P(None, "tp"),
            P(),
            P(),
            P(None, None, "tp"),
            P(None, None, "tp"),
            P(None, "tp"),
            P(None, "tp"),
            P(None, "tp"),
            P(None, "tp", None),
            P(None, "tp", None),
            P(None, "tp", None),
            P(None, "tp", None),
            P(None, "tp"),
            P(None, None, "tp"),
            P(None, None, "tp"),
            P(None, "tp", None),
            P(None, None, "tp"),
            P(None, None, "tp"),
        ),
        out_specs=(P(None, "tp"), P(None, None, "tp"), P(None, None, "tp")),
        check_vma=False,
    )
```
